32 devices in a mesh: ep: 8 (over z, core), tp: 4 (over y, x).
Axes of the slice: x: 2, y: 2, z: 4, core: 2. Of those that a mesh axis runs over, the one named last changes fastest.
Arguments:
- value_in: bfloat16 [8192, 1536], P('ep', 'tp'), may hold values from -6 to 6
- gate_in: bfloat16 [8192, 1536], P('ep', 'tp'), may hold values from -9 to 9
- conv_kernel: float32 [31, 1536], P(None, 'tp'), may hold values from -40 to 40
- norm_gain: float32 [1536], replicated, may hold values from 0.1 to 1.9
- norm_shift: float32 [1536], replicated, may hold values from -3 to 3
- out_weight: bfloat16 [1536, 2048], P(None, 'tp'), may hold values from -0.15625 to 0.15625
- expert_input: bfloat16 [1536, 2048], P('ep'), may hold values from -6 to 6
- expert_gain: float32 [2048], replicated, may hold values from 0.1 to 1.9
- route_ids: int32 [1536, 4], P('ep'), may hold values from 0 to 7, all different within a row; in each aligned block of 192 rows (0 to 191, 192 to 383, ...) at most 120 rows name the same one
- route_weights: float32 [1536, 4], P('ep'), may hold values from 0.2 to 1
- gate_weight: bfloat16 [8, 2048, 2048], P('ep', None, 'tp'), may hold values from -0.375 to 0.375
- up_weight: bfloat16 [8, 2048, 2048], P('ep', None, 'tp'), may hold values from -0.375 to 0.375
- down_weight: bfloat16 [8, 2048, 2048], P('ep', None, 'tp'), may hold values from -0.01953125 to 0.01953125
Outputs:
- mixed_out: bfloat16 [8192, 2048], P('ep', 'tp')
- routed_out: bfloat16 [1536, 2048], P('ep', 'tp')
The draws below stay inside these ranges and needn't reach their ends.
Inputs may be any that keep to these rules, and one draw needn't show every extreme that they name: `route_ids`: each row names 4 different experts; among the rows of one index of ep (aligned blocks of 192 rows) no expert is named by more than 120 rows, and in some block one expert is named by exactly 120.
All inputs are finite; a program needn't handle non-finite values.
Results may differ from the reference program's by a relative error of at most 0.0071.
Values may be sent and summed in bfloat16 or wider, within the bound.
A program may use at most 64 MiB of HBM per device.

```python
import math
import jax
import jax.numpy as jnp
import numpy as np
from jax import lax

D = 2048
CH = 1536
FF = 2048
KW = 31
TOPK = 4
TOK_B = 192
EXPERTS = 8
CAP = 120
LENGTH = 8192
TOKENS_B = 1536
N_EP = 8


def draw_conv_kernel(key, part):
    first_key, second_key = jax.random.split(jax.random.fold_in(key, 17), 2)
    channel = jnp.arange(CH, dtype=jnp.float32) / CH
    jitter = jax.random.uniform(second_key, (CH,), jnp.float32, 0.0, 1.0)
    entries = jnp.clip(jax.random.normal(first_key, (KW, CH), jnp.float32), -4.0, 4.0)
    scales = 10.0 ** channel * 2.0 ** jitter
    return (entries * scales[None, :] * KW ** (-0.5)).astype(jnp.float32)


def steps_of(rng, extent, pieces, smallest, top_value):
    def one(dim, blocks):
        draws = jax.random.uniform(jax.random.fold_in(jax.random.fold_in(rng, 6), dim), (blocks,), jnp.float32, smallest / len(pieces), top_value / len(pieces))
        return jnp.repeat(jnp.exp(draws), extent[dim] // blocks).reshape((-1,) + (1,) * (len(extent) - dim - 1))

    factor_of = one(*pieces[0])
    for cut in pieces[1:]:
        factor_of = factor_of * one(*cut)
    return factor_of


def assign_block(key, own, number, rows, number_of, top, bound, lean):
    sequence = jax.random.permutation(key, number_of)
    packed, common = portions_of(number_of, rows * top, bound, lean, True), portions_of(number_of, rows * top, bound, lean, False)
    places = jnp.arange(number_of)

    def named(tallies, turn):
        used = int((tallies > 0).sum())
        fixed = max(1, used // 4)
        passed = fixed + (places - fixed + turn * (used - fixed)) % max(1, number_of - fixed)
        return jnp.zeros((number_of,), jnp.int32).at[sequence[jnp.where(places < fixed, places, passed)]].set(jnp.asarray(tallies, jnp.int32))

    tallies = jnp.where(number % 4 == 0, named(packed, number // 4), named(common, number - number // 4 - 1))
    mixed = jax.random.permutation(jax.random.fold_in(own, 3), number_of)
    donor, receiver = mixed[0:number_of // 2 * 2:2], mixed[1:number_of // 2 * 2:2]
    margin = jnp.minimum(tallies[donor] - 1, bound - tallies[receiver]) // 2
    margin = jnp.where((donor == sequence[0]) | (receiver == sequence[0]) | (tallies[receiver] == 0), 0, jnp.maximum(margin, 0))
    passed = jax.random.randint(jax.random.fold_in(own, 4), (number_of // 2,), 0, 1 << 20) % (margin + 1)
    tallies = tallies.at[donor].add(-passed).at[receiver].add(passed)
    members = jnp.searchsorted(jnp.cumsum(tallies), jnp.arange(rows * top), side="right").astype(jnp.int32)
    grid = members.reshape(top, rows).T
    grid = grid[jax.random.permutation(jax.random.fold_in(own, 1), rows)]
    turn = jax.random.randint(jax.random.fold_in(own, 2), (rows, 1), 0, top)
    return jnp.take_along_axis(grid, (jnp.arange(top)[None, :] + turn) % top, axis=1)


def portions_of(amount, total, limit, skew, full):
    portions = [(1 << 20) // math.isqrt(rank ** skew) + 1 for rank in range(1, amount + 1)]
    largest = limit if full else min(limit, max(-(-total // amount), total * portions[0] // sum(portions)))
    least = 1 if total - largest >= amount - 1 else 0
    given, rest = [largest] + [least] * (amount - 1), total - largest - least * (amount - 1)
    while rest > 0:
        free = [i for i in range(1, amount) if given[i] < largest] or [i for i in range(1, amount) if given[i] < limit]
        pool, remaining = sum([portions[i] for i in free]), rest
        for i in free:
            extra = min(limit - given[i], max(1, remaining * portions[i] // pool), rest)
            given[i] = given[i] + extra
            rest = rest - extra
    return np.array(given)


def gaussian(own_key, shape, width, limit, cuts=(), kind=jnp.bfloat16):
    values = jax.random.normal(own_key, shape, jnp.float32) * width
    if len(cuts) > 0:
        values = steps_of(own_key, shape, cuts, -0.22, 0.18) * values
    return jnp.clip(values, min=-limit, max=limit).astype(kind)


def setup_inputs(seed: int = 0) -> dict:
    key_list = jax.random.split(jax.random.key(seed), 14)
    value_in = gaussian(key_list[0], (LENGTH, CH), 1.0, 6.0, ((0, 8), (1, 4)))
    gate_in = gaussian(key_list[1], (LENGTH, CH), 1.5, 9.0, ((0, 8), (1, 4)))
    conv_kernel = draw_conv_kernel(jax.random.fold_in(key_list[13], 71), 0)
    norm_gain = jnp.clip(1.0 + 0.18 * jax.random.normal(key_list[3], (CH,), jnp.float32), 0.1, 1.9)
    norm_shift = gaussian(key_list[4], (CH,), 0.5, 3.0, (), jnp.float32)
    out_weight = gaussian(key_list[5], (CH, D), CH ** -0.5, 0.15625, ((1, 4),))
    expert_input = gaussian(key_list[6], (TOKENS_B, D), 1.0, 6.0, ((0, 8),))
    expert_gain = jnp.clip(1.0 + 0.18 * jax.random.normal(key_list[7], (D,), jnp.float32), 0.1, 1.9)
    route_ids_keys = jax.random.split(jax.random.fold_in(key_list[8], 1), TOKENS_B // TOK_B)
    route_ids_turns = jax.random.permutation(jax.random.fold_in(key_list[8], 3), TOKENS_B // TOK_B)
    route_ids = jax.vmap(lambda own, number: assign_block(jax.random.fold_in(key_list[8], 2), own, number, TOK_B, EXPERTS, TOPK, CAP, 2))(route_ids_keys, route_ids_turns).reshape((TOKENS_B, TOPK))
    route_weights = jnp.clip(0.2 + 0.8 * jax.random.uniform(key_list[9], (TOKENS_B, TOPK), jnp.float32) ** steps_of(key_list[9], (TOKENS_B, TOPK), ((0, 8),), -0.2, 0.2), 0.2, 1.0)
    gate_weight = gaussian(key_list[10], (EXPERTS, D, FF), (D // 9) ** -0.5, 0.375, ((0, 8), (2, 4)))
    up_weight = gaussian(key_list[11], (EXPERTS, D, FF), (D // 9) ** -0.5, 0.375, ((0, 8), (2, 4)))
    down_weight = gaussian(key_list[12], (EXPERTS, FF, D), (45 * FF) ** -0.5, 0.01953125, ((0, 8), (2, 4)))
    return {"value_in": value_in, "gate_in": gate_in, "conv_kernel": conv_kernel, "norm_gain": norm_gain, "norm_shift": norm_shift, "out_weight": out_weight, "expert_input": expert_input, "expert_gain": expert_gain, "route_ids": route_ids, "route_weights": route_weights, "gate_weight": gate_weight, "up_weight": up_weight, "down_weight": down_weight}


def reference(value_in, gate_in, conv_kernel, norm_gain, norm_shift, out_weight, expert_input, expert_gain, route_ids, route_weights, gate_weight, up_weight, down_weight):
    gated_values = (value_in.astype(jnp.float32) * jax.nn.sigmoid(gate_in.astype(jnp.float32))).astype(jnp.bfloat16)
    kernel_width = conv_kernel.shape[0]
    positions = gated_values.shape[0]
    padded = jnp.concatenate([jnp.zeros((kernel_width - 1, gated_values.shape[1]), jnp.bfloat16), gated_values], 0)
    running = jnp.zeros(gated_values.shape, jnp.float32)
    for tap_index in range(kernel_width):
        running = running + conv_kernel[tap_index][None, :] * padded[tap_index:tap_index + positions].astype(jnp.float32)
    convolved = running.astype(jnp.bfloat16)
    conv_float = convolved.astype(jnp.float32)
    row_mean = lax.optimization_barrier(jnp.mean(conv_float, axis=1, keepdims=True))
    row_var = lax.optimization_barrier(jnp.mean(jnp.square(conv_float - row_mean), axis=1, keepdims=True))
    normed = (conv_float - row_mean) * lax.rsqrt(row_var + 1e-05) * norm_gain[None, :] + norm_shift[None, :]
    hidden = jax.nn.silu(normed).astype(jnp.bfloat16)
    mixed_out = jnp.dot(hidden, out_weight, preferred_element_type=jnp.float32).astype(jnp.bfloat16)
    input_float = expert_input.astype(jnp.float32)
    feature_mean = lax.optimization_barrier(jnp.mean(input_float, axis=1, keepdims=True))
    feature_var = lax.optimization_barrier(jnp.mean(jnp.square(input_float - feature_mean), axis=1, keepdims=True))
    normed_rows = ((input_float - feature_mean) * lax.rsqrt(feature_var + 1e-05) * expert_gain[None, :]).astype(jnp.bfloat16)
    row_total = expert_input.shape[0]
    block_ids = route_ids.reshape(N_EP, TOK_B * TOPK)
    onehot = (block_ids[:, :, None] == jnp.arange(EXPERTS, dtype=jnp.int32)[None, None, :]).astype(jnp.int32)
    earlier = jnp.cumsum(onehot, axis=1) - onehot
    position = lax.optimization_barrier(jnp.sum(earlier * onehot, axis=2))
    blocks = jnp.arange(N_EP, dtype=jnp.int32)[:, None]
    slot_index = (block_ids * (N_EP * CAP) + blocks * CAP + position).reshape(-1).astype(jnp.int32)
    token_index = jnp.arange(N_EP * TOK_B * TOPK, dtype=jnp.int32) // TOPK
    slot_table = jnp.full((EXPERTS * N_EP * CAP,), row_total, jnp.int32).at[slot_index].set(token_index)
    padded_rows = jnp.concatenate([normed_rows, jnp.zeros((1, normed_rows.shape[1]), jnp.bfloat16)], 0)

    def run_expert(operands):
        table_rows, gate_matrix, up_matrix, down_matrix = operands
        slot_rows = padded_rows[table_rows]
        gate_pre = jnp.dot(slot_rows, gate_matrix, preferred_element_type=jnp.float32)
        up_pre = jnp.dot(slot_rows, up_matrix, preferred_element_type=jnp.float32)
        clamped = jnp.minimum(gate_pre, 7.0)
        upward = jnp.clip(up_pre, -7.0, 7.0)
        activation = ((upward + 1.0) * clamped * jax.nn.sigmoid(1.702 * clamped)).astype(jnp.bfloat16)
        return jnp.dot(activation, down_matrix, preferred_element_type=jnp.float32).astype(jnp.bfloat16)
    results = lax.map(run_expert, (slot_table.reshape(EXPERTS, N_EP * CAP), gate_weight, up_weight, down_weight))
    picked = results.reshape(-1, results.shape[2])[slot_index].reshape(row_total, TOPK, -1).astype(jnp.float32)
    routed_out = lax.optimization_barrier(jnp.sum(picked * route_weights[:, :, None], axis=1)).astype(jnp.bfloat16)
    return (mixed_out, routed_out)
```

```python
import functools

import jax
import jax.numpy as jnp
from jax import lax
from jax.experimental import pallas as pl
from jax.experimental.pallas import tpu as pltpu
from jax.sharding import PartitionSpec as P

MESH = pl.DeviceIdType.MESH
F32 = jnp.float32
BF16 = jnp.bfloat16
HALO = 32


def up_to(value, step):
    return (value + step - 1) // step * step


def half_sigmoid(v):
    return 0.5 + 0.5 * jnp.tanh(0.5 * v)


def kernel(
    cfg,
    value_ref,
    gate_ref,
    taps_ref,
    gain_ref,
    shift_ref,
    rows_ref,
    row_gain_ref,
    ids_ref,
    ids_t_ref,
    route_w_ref,
    out_w_hbm,
    gate_w_hbm,
    up_w_hbm,
    down_w_hbm,
    mixed_ref,
    routed_ref,
    ext,
    conv,
    hidden,
    rows_all,
    slots,
    acts,
    res,
    ret,
    out_w,
    gate_w,
    up_w,
    down_w,
    w_sem,
    halo_sem,
    conv_s,
    conv_r,
    rows_s,
    rows_r,
    act_s,
    act_r,
    ret_s,
    ret_r,
):
    n_ep, n_tp, taps, nk, slot, experts = cfg
    n_z = n_ep // 2
    me = lax.axis_index("ep")
    t = lax.axis_index("tp")
    p = me // 2
    c = me % 2
    tx = t + 1 - 2 * (t % 2)
    ty = t + 2 - 4 * (t // 2)
    td = 3 - t
    length, ch = value_ref.shape
    groups = ch // 128
    n_rows, width = rows_ref.shape
    half_ff = gate_w.shape[1]
    cols_out = out_w.shape[1]
    chunk = length // nk
    tile = 256
    pending = []

    loads = []
    for i, (src, dst) in enumerate(
        ((gate_w_hbm.at[0], gate_w), (up_w_hbm.at[0], up_w), (out_w_hbm, out_w), (down_w_hbm.at[0], down_w))
    ):
        copy = pltpu.make_async_copy(src, dst, w_sem.at[i])
        copy.start()
        loads.append(copy)

    barrier = pltpu.get_barrier_semaphore()
    for i in range(1, n_ep):
        pl.semaphore_signal(
            barrier, inc=1, device_id={"ep": (me + i) % n_ep}, device_id_type=MESH
        )
    for other in (tx, ty):
        pl.semaphore_signal(barrier, inc=1, device_id={"tp": other}, device_id_type=MESH)

    def send(src, dst, ss, rs, dev, cond=None):
        def make():
            return pltpu.make_async_remote_copy(
                src_ref=src,
                dst_ref=dst,
                send_sem=ss,
                recv_sem=rs,
                device_id=dev,
                device_id_type=MESH,
            )

        if cond is None:
            make().start()
        else:

            @pl.when(cond)
            def _():
                make().start()

        pending.append((make, cond))

    def arrived(ref, ss, rs, cond=None):
        def wait():
            pltpu.make_async_remote_copy(
                src_ref=ref,
                dst_ref=ref,
                send_sem=ss,
                recv_sem=rs,
                device_id={"tp": tx},
                device_id_type=MESH,
            ).wait_recv()

        if cond is None:
            wait()
        else:
            pl.when(cond)(wait)

    def gated_step(i, _):
        r = pl.multiple_of(i * 32, 32)
        for g in range(groups):
            lanes = slice(g * 128, (g + 1) * 128)
            v = value_ref[pl.ds(r, 32), lanes].astype(F32)
            s = half_sigmoid(gate_ref[pl.ds(r, 32), lanes].astype(F32))
            ext[g, pl.ds(HALO + r, 32), :] = (v * s).astype(BF16).astype(F32)
        return 0

    lax.fori_loop(0, length // 32, gated_step, 0)

    def norm_step(i, _):
        r = pl.multiple_of(i * 16, 16)
        x = rows_ref[pl.ds(r, 16), :].astype(F32)
        mean = jnp.mean(x, axis=1, keepdims=True)
        d = x - mean
        var = jnp.mean(d * d, axis=1, keepdims=True)
        rows_all[p, c, pl.ds(r, 16), :] = (d * lax.rsqrt(var + 1e-05) * row_gain_ref[...]).astype(BF16)
        return 0

    lax.fori_loop(0, n_rows // 16, norm_step, 0)
    extra = rows_all.shape[2] - n_rows
    lanes_t = ids_t_ref.shape[1]
    e_iota = lax.broadcasted_iota(jnp.int32, (extra, lanes_t), 0)
    named_t = jnp.zeros((extra, lanes_t), F32)
    for k in range(ids_t_ref.shape[0]):
        named_t += jnp.where(ids_t_ref[k : k + 1, :] == e_iota, 1.0, 0.0)
    before_t = jnp.where(
        lax.broadcasted_iota(jnp.int32, (lanes_t, lanes_t), 0)
        < lax.broadcasted_iota(jnp.int32, (lanes_t, lanes_t), 1),
        1.0,
        0.0,
    ).astype(BF16)
    pos_t = jnp.dot(named_t.astype(BF16), before_t, preferred_element_type=F32)
    rows_all[p, c, n_rows : n_rows + extra, :] = jnp.zeros((extra, width), BF16)
    rows_all[p, c, n_rows : n_rows + extra, 0:lanes_t] = jnp.where(named_t > 0.5, pos_t, -1.0).astype(BF16)

    pl.semaphore_wait(barrier, n_ep - 1 + 2)

    tail = ext.at[:, pl.ds(length, HALO), :]
    head = ext.at[:, pl.ds(0, HALO), :]
    send(tail, head, halo_sem.at[0], halo_sem.at[1], {"ep": (me + 1) % n_ep}, me < n_ep - 1)

    def send_rows(q, up, down):
        block = rows_all.at[q, c]
        send(block, block, rows_s.at[q, 0], rows_r.at[q, c], {"ep": (me + 2) % n_ep}, up)
        send(block, block, rows_s.at[q, 1], rows_r.at[q, c], {"ep": (me + n_ep - 2) % n_ep}, down)
        exists = jnp.logical_or(up, down)
        return block, exists

    def to_partner(q, cond):
        block = rows_all.at[q, c]
        send(block, block, rows_s.at[q, 2], rows_r.at[q, c], {"ep": me + 1 - 2 * c}, cond)

    send_rows(p, p < n_z - 1, p > 0)
    to_partner(p, None)

    @pl.when(me == 0)
    def _():
        ext[:, 0:HALO, :] = jnp.zeros((groups, HALO, 128), F32)

    def conv_chunk(k):
        for g in range(groups):
            lanes = slice(g * 128, (g + 1) * 128)
            weights = [taps_ref[j : j + 1, lanes] for j in range(taps)]

            def step(i, _):
                r = pl.multiple_of(k * chunk + i * 64, 64)
                total = weights[0] * ext[g, pl.ds(r + HALO - taps + 1, 64), :]
                for j in range(1, taps):
                    total += weights[j] * ext[g, pl.ds(r + HALO - taps + 1 + j, 64), :]
                conv[t, pl.ds(r, 64), lanes] = total.astype(BF16)
                return 0

            lax.fori_loop(0, chunk // 64, step, 0)
        part = conv.at[t, pl.ds(k * chunk, chunk), :]
        send(part, part, conv_s.at[0, k], conv_r.at[t, k], {"tp": tx})
        send(part, part, conv_s.at[1, k], conv_r.at[t, k], {"tp": ty})

    order = list(range(1, nk)) + [0]
    for k in order:
        if k == 0:
            arrived(head, halo_sem.at[0], halo_sem.at[1], me > 0)
        conv_chunk(k)

    def conv_relay(k):
        rows = pl.ds(k * chunk, chunk)
        for source in (tx, ty):
            arrived(conv.at[source, rows, :], conv_s.at[0, k], conv_r.at[source, k])
        source, target = (tx, ty) if k % 2 == 0 else (ty, tx)
        part = conv.at[source, rows, :]
        send(part, part, conv_s.at[2, k], conv_r.at[source, k], {"tp": target})

    def project(k):
        arrived(conv.at[td, pl.ds(k * chunk, chunk), :], conv_s.at[0, k], conv_r.at[td, k])

        def step(i, _):
            r = pl.multiple_of(k * chunk + i * 16, 16)
            h = pl.multiple_of(i * 16, 16)
            parts = [conv[u, pl.ds(r, 16), :].astype(F32) for u in range(n_tp)]
            mean = sum(jnp.sum(x, axis=1, keepdims=True) for x in parts) / (n_tp * ch)
            parts = [x - mean for x in parts]
            var = sum(jnp.sum(x * x, axis=1, keepdims=True) for x in parts) / (n_tp * ch)
            scale = lax.rsqrt(var + 1e-05)
            for u in range(n_tp):
                v = parts[u] * scale * gain_ref[u : u + 1, :] + shift_ref[u : u + 1, :]
                hidden[pl.ds(h, 16), u * ch : (u + 1) * ch] = (v * half_sigmoid(v)).astype(BF16)
            return 0

        lax.fori_loop(0, chunk // 16, step, 0, unroll=2)

        def cols(i, _):
            o = pl.multiple_of(i * tile, tile)
            mixed_ref[k * chunk : (k + 1) * chunk, pl.ds(o, tile)] = jnp.dot(
                hidden[...], out_w[:, pl.ds(o, tile)], preferred_element_type=F32
            ).astype(BF16)
            return 0

        lax.fori_loop(0, cols_out // tile, cols, 0)

    less = jnp.minimum(p, n_z - 1 - p)
    longer_up = jnp.where(p <= n_z - 1 - p, 1, -1)

    def chip_of(j):
        near = p + (j + 1) // 2 * (-1 if j % 2 else 1)
        return jnp.where(j <= 2 * less, near, p + longer_up * (j - less))

    def rows_relay(d):
        below, above = p - d, p + d
        low = jnp.maximum(below, 0)
        high = jnp.minimum(above, n_z - 1)
        has_low, has_high = below >= 0, above <= n_z - 1
        for q, has, step, onward in (
            (low, has_low, 2, jnp.logical_and(has_low, p < n_z - 1)),
            (high, has_high, n_ep - 2, jnp.logical_and(has_high, p > 0)),
        ):
            block = rows_all.at[q, c]
            arrived(block, rows_s.at[q, 0], rows_r.at[q, c], has)
            send(block, block, rows_s.at[q, 0], rows_r.at[q, c], {"ep": (me + step) % n_ep}, onward)
            to_partner(q, has)

    def act_part(source, q, h):
        return acts.at[source, q, pl.ds(h * slot, slot), :]

    def expert_up(j):
        q = chip_of(j)
        arrived(rows_all.at[q, 1 - c], rows_s.at[q, 0], rows_r.at[q, 1 - c])
        for h in range(2):
            marks = rows_all[q, h, n_rows : n_rows + extra, 0:lanes_t].astype(F32)
            mine = jnp.sum(jnp.where(e_iota == me, marks, 0.0), axis=0, keepdims=True)[:, :n_rows]
            pick = jnp.where(
                lax.broadcasted_iota(jnp.int32, (slot, n_rows), 0).astype(F32) == mine, 1.0, 0.0
            ).astype(BF16)

            def gather(i, _):
                o = pl.multiple_of(i * tile, tile)
                slots[h * slot : (h + 1) * slot, pl.ds(o, tile)] = jnp.dot(
                    pick, rows_all[q, h, 0:n_rows, pl.ds(o, tile)], preferred_element_type=F32
                ).astype(BF16)
                return 0

            lax.fori_loop(0, width // tile, gather, 0)
        if j == 0:
            loads[0].wait()
            loads[1].wait()

        def cols(i, _):
            o = pl.multiple_of(i * tile, tile)
            x = slots[...]
            gate = jnp.dot(x, gate_w[:, pl.ds(o, tile)], preferred_element_type=F32)
            up = jnp.dot(x, up_w[:, pl.ds(o, tile)], preferred_element_type=F32)
            gate = jnp.minimum(gate, 7.0)
            up = jnp.clip(up, -7.0, 7.0)
            acts[t, q, :, pl.ds(o, tile)] = ((up + 1.0) * gate * half_sigmoid(1.702 * gate)).astype(BF16)
            return 0

        lax.fori_loop(0, half_ff // tile, cols, 0)
        for h in range(2):
            part = act_part(t, q, h)
            send(part, part, act_s.at[0, q, h], act_r.at[t, q, h], {"tp": tx})
            send(part, part, act_s.at[1, q, h], act_r.at[t, q, h], {"tp": ty})

    def act_relay(j):
        q = chip_of(j)
        for h, source, target in ((0, tx, ty), (1, ty, tx)):
            part = act_part(source, q, h)
            arrived(part, act_s.at[0, q, h], act_r.at[source, q, h])
            send(part, part, act_s.at[2, q, h], act_r.at[source, q, h], {"tp": target})

    def expert_down(j):
        q = chip_of(j)
        for source, h in ((tx, 1), (ty, 0), (td, 0), (td, 1)):
            arrived(act_part(source, q, h), act_s.at[0, q, h], act_r.at[source, q, h])
        if j == 0:
            loads[3].wait()

        def cols(i, _):
            o = pl.multiple_of(i * tile, tile)
            total = jnp.zeros((2 * slot, tile), F32)
            for u in range(n_tp):
                total += jnp.dot(
                    acts[u, q],
                    down_w[u * half_ff : (u + 1) * half_ff, pl.ds(o, tile)],
                    preferred_element_type=F32,
                )
            res[q, :, pl.ds(o, tile)] = total.astype(BF16)
            return 0

        lax.fori_loop(0, cols_out // tile, cols, 0)
        for h in range(2):
            target = 2 * q + h
            part = res.at[q, pl.ds(h * slot, slot), :]
            send(part, ret.at[me], ret_s.at[target], ret_r.at[me], {"ep": target}, target != me)
        if j == 0:
            for h in range(2):

                @pl.when(c == h)
                def _():
                    ret[me] = res[p, h * slot : (h + 1) * slot, :]

    expert_up(0)
    half = nk // 2
    for k in order[:half]:
        conv_relay(k)
    if n_z > 1:
        rows_relay(1)
        expert_up(1)
    for k in order[half:]:
        conv_relay(k)
    act_relay(0)
    loads[2].wait()
    waiting = list(order)
    for _ in range(half):
        project(waiting.pop(0))
    if n_z > 1:
        act_relay(1)
    for j in range(2, n_z):
        rows_relay(j)
        expert_up(j)
        if waiting:
            project(waiting.pop(0))
        expert_down(j - 2)
        act_relay(j)
    for k in waiting:
        project(k)
    for j in range(max(0, n_z - 2), n_z):
        expert_down(j)

    lane_e = lax.broadcasted_iota(jnp.int32, (n_rows, 128), 1)
    named = jnp.zeros((n_rows, 128), F32)
    share = jnp.zeros((n_rows, 128), F32)
    for k in range(ids_ref.shape[1]):
        hit = ids_ref[:, k : k + 1] == lane_e
        named += jnp.where(hit, 1.0, 0.0)
        share += jnp.where(hit, route_w_ref[:, k : k + 1], 0.0)
    before = jnp.where(
        lax.broadcasted_iota(jnp.int32, (n_rows, n_rows), 1)
        < lax.broadcasted_iota(jnp.int32, (n_rows, n_rows), 0),
        1.0,
        0.0,
    ).astype(BF16)
    pos = jnp.dot(before, named.astype(BF16), preferred_element_type=F32)
    pos = jnp.where(named > 0.5, pos, -1.0)
    slot_iota = lax.broadcasted_iota(jnp.int32, (n_rows, slot), 1).astype(F32)
    total = jnp.zeros((n_rows, cols_out), F32)
    for e in range(experts):
        arrived(ret.at[e], ret_s.at[e], ret_r.at[e], me != e)
        combine = jnp.where(pos[:, e : e + 1] == slot_iota, share[:, e : e + 1], 0.0)
        high = combine.astype(BF16)
        low = (combine - high.astype(F32)).astype(BF16)
        back = ret[e]
        total += jnp.dot(high, back, preferred_element_type=F32)
        total += jnp.dot(low, back, preferred_element_type=F32)
    routed_ref[...] = total.astype(BF16)

    for make, cond in pending:
        if cond is None:
            make().wait_send()
        else:

            @pl.when(cond)
            def _(make=make):
                make().wait_send()


def shifted(block, axis, distance):
    devices = range(lax.axis_size(axis))
    route = [(i - distance, i) for i in devices if i - distance in devices]
    return lax.ppermute(block, axis, route)


def expert_tail(gate_pre, up_pre, down_weight):
    clamped = jnp.minimum(gate_pre, 7.0)
    upward = jnp.clip(up_pre, -7.0, 7.0)
    activation = ((upward + 1.0) * clamped * jax.nn.sigmoid(1.702 * clamped)).astype(jnp.bfloat16)
    weights = down_weight[0]
    summed = jnp.dot(
        lax.all_gather(activation, "tp", axis=1, tiled=True),
        weights,
        preferred_element_type=jnp.float32,
    )
    return summed.astype(jnp.bfloat16)


def finish(gate_pre, up_pre, down_weight, arrived_shape):
    outcome = expert_tail(gate_pre, up_pre, down_weight)
    outcome = outcome.reshape(arrived_shape[0], arrived_shape[1], outcome.shape[1])
    return lax.all_to_all(outcome, "ep", split_axis=0, concat_axis=0, tiled=True)


def plain_body(
    value_in,
    gate_in,
    conv_kernel,
    norm_gain,
    norm_shift,
    out_weight,
    expert_input,
    expert_gain,
    route_ids,
    route_weights,
    gate_weight,
    up_weight,
    down_weight,
):
    gated_values = (
        value_in.astype(jnp.float32) * jax.nn.sigmoid(gate_in.astype(jnp.float32))
    ).astype(jnp.bfloat16)
    kernel_width = conv_kernel.shape[0]
    length_dev = gated_values.shape[0]
    before = shifted(gated_values[length_dev - (kernel_width - 1) :], "ep", 1)
    extended = jnp.concatenate([before, gated_values], 0).astype(jnp.float32)
    running = jnp.zeros(gated_values.shape, jnp.float32)
    for tap_index in range(kernel_width):
        running = (
            running + conv_kernel[tap_index][None, :] * extended[tap_index : tap_index + length_dev]
        )
    convolved = running.astype(jnp.bfloat16)
    gathered = lax.all_gather(convolved, "tp", axis=1, tiled=True).astype(jnp.float32)
    row_mean = jnp.mean(gathered, axis=1, keepdims=True)
    row_var = jnp.mean(jnp.square(gathered - row_mean), axis=1, keepdims=True)
    normed = (gathered - row_mean) * lax.rsqrt(row_var + 1e-05) * norm_gain[None, :] + norm_shift[
        None, :
    ]
    hidden = jax.nn.silu(normed).astype(jnp.bfloat16)
    mixed_out = jnp.dot(hidden, out_weight, preferred_element_type=jnp.float32).astype(jnp.bfloat16)
    experts = lax.axis_size("ep")
    row_count, model_width = expert_input.shape
    top_count = route_ids.shape[1]
    capacity = (5 * row_count * top_count + 4 * experts - 1) // (4 * experts)
    input_float = expert_input.astype(jnp.float32)
    feature_mean = jnp.mean(input_float, axis=1, keepdims=True)
    feature_var = jnp.mean(jnp.square(input_float - feature_mean), axis=1, keepdims=True)
    normed_rows = (
        (input_float - feature_mean) * lax.rsqrt(feature_var + 1e-05) * expert_gain[None, :]
    ).astype(jnp.bfloat16)
    expert_ids = route_ids.reshape(-1)
    onehot = (expert_ids[:, None] == jnp.arange(experts, dtype=jnp.int32)[None, :]).astype(
        jnp.int32
    )
    earlier = jnp.cumsum(onehot, axis=0) - onehot
    position = jnp.sum(earlier * onehot, axis=1)
    destination = expert_ids * capacity + position
    token_index = jnp.arange(expert_ids.shape[0], dtype=jnp.int32) // top_count
    slot_token = (
        jnp.full((experts * capacity,), row_count, jnp.int32).at[destination].set(token_index)
    )
    padded = jnp.concatenate([normed_rows, jnp.zeros((1, model_width), jnp.bfloat16)], 0)
    outgoing = padded[slot_token].reshape(experts, capacity, model_width)
    column_width = model_width // lax.axis_size("tp")
    columns = lax.dynamic_slice_in_dim(
        outgoing, lax.axis_index("tp") * column_width, column_width, 2
    )
    arrived = lax.all_to_all(columns, "ep", split_axis=0, concat_axis=0, tiled=True)
    slot_total = arrived.shape[0] * arrived.shape[1]
    portion = lax.all_gather(arrived, "tp", axis=2, tiled=True)
    flattened = portion.reshape(slot_total, portion.shape[2])
    gate_part = gate_weight[0]
    up_part = up_weight[0]
    gate_pre = jnp.dot(flattened, gate_part, preferred_element_type=jnp.float32)
    up_pre = jnp.dot(flattened, up_part, preferred_element_type=jnp.float32)
    results_home = finish(gate_pre, up_pre, down_weight, arrived.shape)
    picked = results_home.reshape(-1, results_home.shape[2])[destination]
    picked = picked.reshape(row_count, top_count, -1).astype(jnp.float32)
    routed_out = jnp.sum(picked * route_weights[:, :, None], axis=1).astype(jnp.bfloat16)
    return (mixed_out, routed_out)


def body(
    value_in,
    gate_in,
    conv_kernel,
    norm_gain,
    norm_shift,
    out_weight,
    expert_input,
    expert_gain,
    route_ids,
    route_weights,
    gate_weight,
    up_weight,
    down_weight,
):
    n_ep, n_tp = lax.axis_size("ep"), lax.axis_size("tp")
    length, ch = value_in.shape
    n_rows, width = expert_input.shape
    top = route_ids.shape[1]
    if n_tp != 4 or ch % 128 or n_ep % 2:
        return plain_body(
            value_in,
            gate_in,
            conv_kernel,
            norm_gain,
            norm_shift,
            out_weight,
            expert_input,
            expert_gain,
            route_ids,
            route_weights,
            gate_weight,
            up_weight,
            down_weight,
        )
    experts = n_ep
    capacity = (5 * n_rows * top + 4 * experts - 1) // (4 * experts)
    slot = up_to(capacity, 16)
    extra = up_to(experts, 16)
    half_ff = gate_weight.shape[2]
    cols_out = out_weight.shape[1]
    down_cols = down_weight.shape[2]
    nk = 4
    n_z = n_ep // 2
    ids_t = jnp.pad(route_ids.T, ((0, 0), (0, up_to(n_rows, 128) - n_rows)), constant_values=-1)
    cfg = (n_ep, n_tp, conv_kernel.shape[0], nk, slot, experts)
    vmem = pl.BlockSpec(memory_space=pltpu.VMEM)
    hbm = pl.BlockSpec(memory_space=pl.ANY)
    dma = pltpu.SemaphoreType.DMA
    return pl.pallas_call(
        functools.partial(kernel, cfg),
        out_shape=(
            jax.ShapeDtypeStruct((length, cols_out), BF16),
            jax.ShapeDtypeStruct((n_rows, down_cols), BF16),
        ),
        in_specs=[vmem] * 10 + [hbm] * 4,
        out_specs=(vmem, vmem),
        scratch_shapes=[
            pltpu.VMEM((ch // 128, HALO + length, 128), F32),
            pltpu.VMEM((n_tp, length, ch), BF16),
            pltpu.VMEM((length // nk, n_tp * ch), BF16),
            pltpu.VMEM((n_z, 2, n_rows + extra, width), BF16),
            pltpu.VMEM((2 * slot, width), BF16),
            pltpu.VMEM((n_tp, n_z, 2 * slot, half_ff), BF16),
            pltpu.VMEM((n_z, 2 * slot, down_cols), BF16),
            pltpu.VMEM((n_ep, slot, down_cols), BF16),
            pltpu.VMEM(out_weight.shape, BF16),
            pltpu.VMEM(gate_weight.shape[1:], BF16),
            pltpu.VMEM(up_weight.shape[1:], BF16),
            pltpu.VMEM(down_weight.shape[1:], BF16),
            dma((4,)),
            dma((2,)),
            dma((3, nk)),
            dma((n_tp, nk)),
            dma((n_z, 3)),
            dma((n_z, 2)),
            dma((3, n_z, 2)),
            dma((n_tp, n_z, 2)),
            dma((n_ep,)),
            dma((n_ep,)),
        ],
        compiler_params=pltpu.CompilerParams(
            collective_id=0, has_side_effects=True, vmem_limit_bytes=62 * 1024 * 1024
        ),
    )(
        value_in,
        gate_in,
        conv_kernel,
        norm_gain.reshape(n_tp, ch),
        norm_shift.reshape(n_tp, ch),
        expert_input,
        expert_gain.reshape(1, width),
        route_ids,
        ids_t,
        route_weights,
        out_weight,
        gate_weight,
        up_weight,
        down_weight,
    )


def solution(mesh):
    return jax.shard_map(
        body,
        mesh=mesh,
        in_specs=(
            P("ep", "tp"),
            P("ep", "tp"),
            P(None, "tp"),
            P(),
            P(),
            P(None, "tp"),
            P("ep", None),
            P(),
            P("ep", None),
            P("ep", None),
            P("ep", None, "tp"),
            P("ep", None, "tp"),
            P("ep", None, "tp"),
        ),
        out_specs=(P("ep", "tp"), P("ep", "tp")),
        check_vma=False,
    )
```

```python
import functools

import jax
import jax.numpy as jnp
from jax import lax
from jax.experimental import pallas as pl
from jax.experimental.pallas import tpu as pltpu
from jax.sharding import PartitionSpec as P

MESH = pl.DeviceIdType.MESH
F32 = jnp.float32
BF16 = jnp.bfloat16
HALO = 32


def up_to(value, step):
    return (value + step - 1) // step * step


def half_sigmoid(v):
    return 0.5 + 0.5 * jnp.tanh(0.5 * v)


def kernel(
    cfg,
    value_ref,
    gate_ref,
    taps_ref,
    gain_ref,
    shift_ref,
    rows_ref,
    row_gain_ref,
    ids_t_ref,
    route_w_ref,
    out_w_hbm,
    gate_w_hbm,
    up_w_hbm,
    down_w_hbm,
    mixed_ref,
    routed_ref,
    ext,
    conv,
    hidden,
    rows_all,
    marks_all,
    route_t,
    slots,
    acts,
    res,
    ret,
    out_w,
    gate_w,
    up_w,
    down_w,
    w_sem,
    halo_sem,
    conv_s,
    conv_r,
    rows_s,
    rows_r,
    mark_s,
    mark_r,
    act_s,
    act_r,
    ret_s,
    ret_r,
):
    n_ep, n_tp, taps, nk, slot, experts = cfg
    n_z = n_ep // 2
    me = lax.axis_index("ep")
    t = lax.axis_index("tp")
    p = me // 2
    c = me % 2
    tx = t + 1 - 2 * (t % 2)
    ty = t + 2 - 4 * (t // 2)
    td = 3 - t
    length, ch = value_ref.shape
    groups = ch // 128
    n_rows, width = rows_ref.shape
    half_ff = gate_w.shape[1]
    cols_out = out_w.shape[1]
    chunk = length // nk
    tile = 256
    pending = []

    loads = []
    for i, (src, dst) in enumerate(
        ((gate_w_hbm.at[0], gate_w), (up_w_hbm.at[0], up_w), (out_w_hbm, out_w), (down_w_hbm.at[0], down_w))
    ):
        copy = pltpu.make_async_copy(src, dst, w_sem.at[i])
        copy.start()
        loads.append(copy)

    barrier = pltpu.get_barrier_semaphore()
    for i in range(1, n_ep):
        pl.semaphore_signal(
            barrier, inc=1, device_id={"ep": (me + i) % n_ep}, device_id_type=MESH
        )
    for other in (tx, ty):
        pl.semaphore_signal(barrier, inc=1, device_id={"tp": other}, device_id_type=MESH)

    def send(src, dst, ss, rs, dev, cond=None):
        def make():
            return pltpu.make_async_remote_copy(
                src_ref=src,
                dst_ref=dst,
                send_sem=ss,
                recv_sem=rs,
                device_id=dev,
                device_id_type=MESH,
            )

        if cond is None:
            make().start()
        else:

            @pl.when(cond)
            def _():
                make().start()

        pending.append((make, cond))

    def arrived(ref, ss, rs, cond=None):
        def wait():
            pltpu.make_async_remote_copy(
                src_ref=ref,
                dst_ref=ref,
                send_sem=ss,
                recv_sem=rs,
                device_id={"tp": tx},
                device_id_type=MESH,
            ).wait_recv()

        if cond is None:
            wait()
        else:
            pl.when(cond)(wait)

    def gated_step(i, _):
        r = pl.multiple_of(i * 32, 32)
        for g in range(groups):
            lanes = slice(g * 128, (g + 1) * 128)
            v = value_ref[pl.ds(r, 32), lanes].astype(F32)
            s = half_sigmoid(gate_ref[pl.ds(r, 32), lanes].astype(F32))
            ext[g, pl.ds(HALO + r, 32), :] = (v * s).astype(BF16).astype(F32)
        return 0

    lax.fori_loop(0, length // 32, gated_step, 0)

    def norm_step(i, _):
        r = pl.multiple_of(i * 16, 16)
        x = rows_ref[pl.ds(r, 16), :].astype(F32)
        mean = jnp.mean(x, axis=1, keepdims=True)
        d = x - mean
        var = jnp.mean(d * d, axis=1, keepdims=True)
        rows_all[p, c, pl.ds(r, 16), :] = (d * lax.rsqrt(var + 1e-05) * row_gain_ref[...]).astype(BF16)
        return 0

    lax.fori_loop(0, n_rows // 16, norm_step, 0)
    extra = marks_all.shape[1]
    e_iota = lax.broadcasted_iota(jnp.int32, (extra, n_rows), 0)
    named_t = jnp.zeros((extra, n_rows), F32)
    share_t = jnp.zeros((extra, n_rows), F32)
    for k in range(ids_t_ref.shape[0]):
        hit = ids_t_ref[k : k + 1, :] == e_iota
        named_t += jnp.where(hit, 1.0, 0.0)
        share_t += jnp.where(hit, route_w_ref[k : k + 1, :], 0.0)
    before_t = jnp.where(
        lax.broadcasted_iota(jnp.int32, (n_rows, n_rows), 0)
        < lax.broadcasted_iota(jnp.int32, (n_rows, n_rows), 1),
        1.0,
        0.0,
    ).astype(BF16)
    pos_t = jnp.dot(named_t.astype(BF16), before_t, preferred_element_type=F32)
    pos_t = jnp.where(named_t > 0.5, pos_t, -1.0)
    marks_all[me] = pos_t.astype(BF16)
    route_t[0] = pos_t
    route_t[1] = share_t

    pl.semaphore_wait(barrier, n_ep - 1 + 2)

    tail = ext.at[:, pl.ds(length, HALO), :]
    head = ext.at[:, pl.ds(0, HALO), :]
    send(tail, head, halo_sem.at[0], halo_sem.at[1], {"ep": (me + 1) % n_ep}, me < n_ep - 1)

    for i in range(1, n_ep):
        other = (me + i) % n_ep
        mark = marks_all.at[me]
        send(mark, mark, mark_s.at[other], mark_r.at[me], {"ep": other})

    def send_rows(q, up, down):
        block = rows_all.at[q, c]
        send(block, block, rows_s.at[q, 0], rows_r.at[q, c], {"ep": (me + 2) % n_ep}, up)
        send(block, block, rows_s.at[q, 1], rows_r.at[q, c], {"ep": (me + n_ep - 2) % n_ep}, down)
        exists = jnp.logical_or(up, down)
        return block, exists

    def to_partner(q, cond):
        block = rows_all.at[q, c]
        send(block, block, rows_s.at[q, 2], rows_r.at[q, c], {"ep": me + 1 - 2 * c}, cond)

    send_rows(p, p < n_z - 1, p > 0)
    to_partner(p, None)

    @pl.when(me == 0)
    def _():
        ext[:, 0:HALO, :] = jnp.zeros((groups, HALO, 128), F32)

    def conv_chunk(k):
        for g in range(groups):
            lanes = slice(g * 128, (g + 1) * 128)
            weights = [taps_ref[j : j + 1, lanes] for j in range(taps)]

            def step(i, _):
                r = pl.multiple_of(k * chunk + i * 64, 64)
                total = weights[0] * ext[g, pl.ds(r + HALO - taps + 1, 64), :]
                for j in range(1, taps):
                    total += weights[j] * ext[g, pl.ds(r + HALO - taps + 1 + j, 64), :]
                conv[t, pl.ds(r, 64), lanes] = total.astype(BF16)
                return 0

            lax.fori_loop(0, chunk // 64, step, 0)
        part = conv.at[t, pl.ds(k * chunk, chunk), :]
        send(part, part, conv_s.at[0, k], conv_r.at[t, k], {"tp": tx})
        send(part, part, conv_s.at[1, k], conv_r.at[t, k], {"tp": ty})

    order = list(range(1, nk)) + [0]
    for k in order:
        if k == 0:
            arrived(head, halo_sem.at[0], halo_sem.at[1], me > 0)
        conv_chunk(k)

    def conv_relay(k):
        rows = pl.ds(k * chunk, chunk)
        for source in (tx, ty):
            arrived(conv.at[source, rows, :], conv_s.at[0, k], conv_r.at[source, k])
        source, target = (tx, ty) if k % 2 == 0 else (ty, tx)
        part = conv.at[source, rows, :]
        send(part, part, conv_s.at[2, k], conv_r.at[source, k], {"tp": target})

    def project(k):
        arrived(conv.at[td, pl.ds(k * chunk, chunk), :], conv_s.at[0, k], conv_r.at[td, k])

        def step(i, _):
            r = pl.multiple_of(k * chunk + i * 16, 16)
            h = pl.multiple_of(i * 16, 16)
            parts = [conv[u, pl.ds(r, 16), :].astype(F32) for u in range(n_tp)]
            mean = sum(jnp.sum(x, axis=1, keepdims=True) for x in parts) / (n_tp * ch)
            parts = [x - mean for x in parts]
            var = sum(jnp.sum(x * x, axis=1, keepdims=True) for x in parts) / (n_tp * ch)
            scale = lax.rsqrt(var + 1e-05)
            for u in range(n_tp):
                v = parts[u] * scale * gain_ref[:, u * ch : (u + 1) * ch] + shift_ref[:, u * ch : (u + 1) * ch]
                hidden[pl.ds(h, 16), u * ch : (u + 1) * ch] = (v * half_sigmoid(v)).astype(BF16)
            return 0

        lax.fori_loop(0, chunk // 16, step, 0, unroll=2)

        def cols(i, _):
            o = pl.multiple_of(i * tile, tile)
            mixed_ref[k * chunk : (k + 1) * chunk, pl.ds(o, tile)] = jnp.dot(
                hidden[...], out_w[:, pl.ds(o, tile)], preferred_element_type=F32
            ).astype(BF16)
            return 0

        lax.fori_loop(0, cols_out // tile, cols, 0)

    less = jnp.minimum(p, n_z - 1 - p)
    longer_up = jnp.where(p <= n_z - 1 - p, 1, -1)

    def chip_of(j):
        near = p + (j + 1) // 2 * (-1 if j % 2 else 1)
        return jnp.where(j <= 2 * less, near, p + longer_up * (j - less))

    def rows_relay(d):
        below, above = p - d, p + d
        low = jnp.maximum(below, 0)
        high = jnp.minimum(above, n_z - 1)
        has_low, has_high = below >= 0, above <= n_z - 1
        for q, has, step, onward in (
            (low, has_low, 2, jnp.logical_and(has_low, p < n_z - 1)),
            (high, has_high, n_ep - 2, jnp.logical_and(has_high, p > 0)),
        ):
            block = rows_all.at[q, c]
            arrived(block, rows_s.at[q, 0], rows_r.at[q, c], has)
            send(block, block, rows_s.at[q, 0], rows_r.at[q, c], {"ep": (me + step) % n_ep}, onward)
            to_partner(q, has)

    def act_part(source, q, h):
        return acts.at[source, q, pl.ds(h * slot, slot), :]

    def expert_up(j):
        q = chip_of(j)
        arrived(rows_all.at[q, 1 - c], rows_s.at[q, 0], rows_r.at[q, 1 - c])
        for h in range(2):
            owner = 2 * q + h
            arrived(marks_all.at[owner], mark_s.at[owner], mark_r.at[owner], owner != me)
            marks = marks_all[owner].astype(F32)
            mine = jnp.sum(jnp.where(e_iota == me, marks, 0.0), axis=0, keepdims=True)
            pick = jnp.where(
                lax.broadcasted_iota(jnp.int32, (slot, n_rows), 0).astype(F32) == mine, 1.0, 0.0
            ).astype(BF16)

            def gather(i, _):
                o = pl.multiple_of(i * tile, tile)
                slots[h * slot : (h + 1) * slot, pl.ds(o, tile)] = jnp.dot(
                    pick, rows_all[q, h, 0:n_rows, pl.ds(o, tile)], preferred_element_type=F32
                ).astype(BF16)
                return 0

            lax.fori_loop(0, width // tile, gather, 0)
        if j == 0:
            loads[0].wait()
            loads[1].wait()

        def cols(i, _):
            o = pl.multiple_of(i * tile, tile)
            x = slots[...]
            gate = jnp.dot(x, gate_w[:, pl.ds(o, tile)], preferred_element_type=F32)
            up = jnp.dot(x, up_w[:, pl.ds(o, tile)], preferred_element_type=F32)
            gate = jnp.minimum(gate, 7.0)
            up = jnp.clip(up, -7.0, 7.0)
            acts[t, q, :, pl.ds(o, tile)] = ((up + 1.0) * gate * half_sigmoid(1.702 * gate)).astype(BF16)
            return 0

        lax.fori_loop(0, half_ff // tile, cols, 0)
        for h in range(2):
            part = act_part(t, q, h)
            send(part, part, act_s.at[0, q, h], act_r.at[t, q, h], {"tp": tx})
            send(part, part, act_s.at[1, q, h], act_r.at[t, q, h], {"tp": ty})

    def act_relay(j):
        q = chip_of(j)
        for h, source, target in ((0, tx, ty), (1, ty, tx)):
            part = act_part(source, q, h)
            arrived(part, act_s.at[0, q, h], act_r.at[source, q, h])
            send(part, part, act_s.at[2, q, h], act_r.at[source, q, h], {"tp": target})

    def expert_down(j):
        q = chip_of(j)
        for source, h in ((tx, 1), (ty, 0), (td, 0), (td, 1)):
            arrived(act_part(source, q, h), act_s.at[0, q, h], act_r.at[source, q, h])
        if j == 0:
            loads[3].wait()

        def cols(i, _):
            o = pl.multiple_of(i * tile, tile)
            total = jnp.zeros((2 * slot, tile), F32)
            for u in range(n_tp):
                total += jnp.dot(
                    acts[u, q],
                    down_w[u * half_ff : (u + 1) * half_ff, pl.ds(o, tile)],
                    preferred_element_type=F32,
                )
            res[q, :, pl.ds(o, tile)] = total.astype(BF16)
            return 0

        lax.fori_loop(0, cols_out // tile, cols, 0)
        for h in range(2):
            target = 2 * q + h
            part = res.at[q, pl.ds(h * slot, slot), :]
            send(part, ret.at[me], ret_s.at[target], ret_r.at[me], {"ep": target}, target != me)
        if j == 0:
            for h in range(2):

                @pl.when(c == h)
                def _():
                    ret[me] = res[p, h * slot : (h + 1) * slot, :]

    expert_up(0)
    half = nk // 2
    for k in order[:half]:
        conv_relay(k)
    if n_z > 1:
        rows_relay(1)
        expert_up(1)
    for k in order[half:]:
        conv_relay(k)
    act_relay(0)
    loads[2].wait()
    waiting = list(order)
    project(waiting.pop(0))
    if n_z > 1:
        act_relay(1)
    done = 0
    for j in range(2, n_z):
        rows_relay(j)
        expert_up(j)
        if j + 1 < n_z:
            while waiting:
                project(waiting.pop(0))
                if done < j:
                    expert_down(done)
                    done += 1
        act_relay(j)
        while done < j + 1:
            expert_down(done)
            done += 1
    while waiting:
        project(waiting.pop(0))
    for j in range(done, n_z):
        expert_down(j)

    slot_iota = lax.broadcasted_iota(jnp.int32, (slot, n_rows), 0).astype(F32)
    over_slots = (((0,), (0,)), ((), ()))
    total = jnp.zeros((n_rows, cols_out), F32)
    for e in range(experts):
        arrived(ret.at[e], ret_s.at[e], ret_r.at[e], me != e)
        combine = jnp.where(route_t[0, e : e + 1, :] == slot_iota, route_t[1, e : e + 1, :], 0.0)
        high = combine.astype(BF16)
        low = (combine - high.astype(F32)).astype(BF16)
        back = ret[e]
        total += lax.dot_general(high, back, over_slots, preferred_element_type=F32)
        total += lax.dot_general(low, back, over_slots, preferred_element_type=F32)
    routed_ref[...] = total.astype(BF16)

    for make, cond in pending:
        if cond is None:
            make().wait_send()
        else:

            @pl.when(cond)
            def _(make=make):
                make().wait_send()


def shifted(block, axis, distance):
    devices = range(lax.axis_size(axis))
    route = [(i - distance, i) for i in devices if i - distance in devices]
    return lax.ppermute(block, axis, route)


def expert_tail(gate_pre, up_pre, down_weight):
    clamped = jnp.minimum(gate_pre, 7.0)
    upward = jnp.clip(up_pre, -7.0, 7.0)
    activation = ((upward + 1.0) * clamped * jax.nn.sigmoid(1.702 * clamped)).astype(jnp.bfloat16)
    weights = down_weight[0]
    summed = jnp.dot(
        lax.all_gather(activation, "tp", axis=1, tiled=True),
        weights,
        preferred_element_type=jnp.float32,
    )
    return summed.astype(jnp.bfloat16)


def finish(gate_pre, up_pre, down_weight, arrived_shape):
    outcome = expert_tail(gate_pre, up_pre, down_weight)
    outcome = outcome.reshape(arrived_shape[0], arrived_shape[1], outcome.shape[1])
    return lax.all_to_all(outcome, "ep", split_axis=0, concat_axis=0, tiled=True)


def plain_body(
    value_in,
    gate_in,
    conv_kernel,
    norm_gain,
    norm_shift,
    out_weight,
    expert_input,
    expert_gain,
    route_ids,
    route_weights,
    gate_weight,
    up_weight,
    down_weight,
):
    gated_values = (
        value_in.astype(jnp.float32) * jax.nn.sigmoid(gate_in.astype(jnp.float32))
    ).astype(jnp.bfloat16)
    kernel_width = conv_kernel.shape[0]
    length_dev = gated_values.shape[0]
    before = shifted(gated_values[length_dev - (kernel_width - 1) :], "ep", 1)
    extended = jnp.concatenate([before, gated_values], 0).astype(jnp.float32)
    running = jnp.zeros(gated_values.shape, jnp.float32)
    for tap_index in range(kernel_width):
        running = (
            running + conv_kernel[tap_index][None, :] * extended[tap_index : tap_index + length_dev]
        )
    convolved = running.astype(jnp.bfloat16)
    gathered = lax.all_gather(convolved, "tp", axis=1, tiled=True).astype(jnp.float32)
    row_mean = jnp.mean(gathered, axis=1, keepdims=True)
    row_var = jnp.mean(jnp.square(gathered - row_mean), axis=1, keepdims=True)
    normed = (gathered - row_mean) * lax.rsqrt(row_var + 1e-05) * norm_gain[None, :] + norm_shift[
        None, :
    ]
    hidden = jax.nn.silu(normed).astype(jnp.bfloat16)
    mixed_out = jnp.dot(hidden, out_weight, preferred_element_type=jnp.float32).astype(jnp.bfloat16)
    experts = lax.axis_size("ep")
    row_count, model_width = expert_input.shape
    top_count = route_ids.shape[1]
    capacity = (5 * row_count * top_count + 4 * experts - 1) // (4 * experts)
    input_float = expert_input.astype(jnp.float32)
    feature_mean = jnp.mean(input_float, axis=1, keepdims=True)
    feature_var = jnp.mean(jnp.square(input_float - feature_mean), axis=1, keepdims=True)
    normed_rows = (
        (input_float - feature_mean) * lax.rsqrt(feature_var + 1e-05) * expert_gain[None, :]
    ).astype(jnp.bfloat16)
    expert_ids = route_ids.reshape(-1)
    onehot = (expert_ids[:, None] == jnp.arange(experts, dtype=jnp.int32)[None, :]).astype(
        jnp.int32
    )
    earlier = jnp.cumsum(onehot, axis=0) - onehot
    position = jnp.sum(earlier * onehot, axis=1)
    destination = expert_ids * capacity + position
    token_index = jnp.arange(expert_ids.shape[0], dtype=jnp.int32) // top_count
    slot_token = (
        jnp.full((experts * capacity,), row_count, jnp.int32).at[destination].set(token_index)
    )
    padded = jnp.concatenate([normed_rows, jnp.zeros((1, model_width), jnp.bfloat16)], 0)
    outgoing = padded[slot_token].reshape(experts, capacity, model_width)
    column_width = model_width // lax.axis_size("tp")
    columns = lax.dynamic_slice_in_dim(
        outgoing, lax.axis_index("tp") * column_width, column_width, 2
    )
    arrived = lax.all_to_all(columns, "ep", split_axis=0, concat_axis=0, tiled=True)
    slot_total = arrived.shape[0] * arrived.shape[1]
    portion = lax.all_gather(arrived, "tp", axis=2, tiled=True)
    flattened = portion.reshape(slot_total, portion.shape[2])
    gate_part = gate_weight[0]
    up_part = up_weight[0]
    gate_pre = jnp.dot(flattened, gate_part, preferred_element_type=jnp.float32)
    up_pre = jnp.dot(flattened, up_part, preferred_element_type=jnp.float32)
    results_home = finish(gate_pre, up_pre, down_weight, arrived.shape)
    picked = results_home.reshape(-1, results_home.shape[2])[destination]
    picked = picked.reshape(row_count, top_count, -1).astype(jnp.float32)
    routed_out = jnp.sum(picked * route_weights[:, :, None], axis=1).astype(jnp.bfloat16)
    return (mixed_out, routed_out)


def body(
    value_in,
    gate_in,
    conv_kernel,
    norm_gain,
    norm_shift,
    out_weight,
    expert_input,
    expert_gain,
    route_ids,
    route_weights,
    gate_weight,
    up_weight,
    down_weight,
):
    n_ep, n_tp = lax.axis_size("ep"), lax.axis_size("tp")
    length, ch = value_in.shape
    n_rows, width = expert_input.shape
    top = route_ids.shape[1]
    if n_tp != 4 or ch % 128 or n_ep % 2:
        return plain_body(
            value_in,
            gate_in,
            conv_kernel,
            norm_gain,
            norm_shift,
            out_weight,
            expert_input,
            expert_gain,
            route_ids,
            route_weights,
            gate_weight,
            up_weight,
            down_weight,
        )
    experts = n_ep
    capacity = (5 * n_rows * top + 4 * experts - 1) // (4 * experts)
    slot = up_to(capacity, 16)
    extra = up_to(experts, 16)
    half_ff = gate_weight.shape[2]
    cols_out = out_weight.shape[1]
    down_cols = down_weight.shape[2]
    nk = 4
    n_z = n_ep // 2
    cfg = (n_ep, n_tp, conv_kernel.shape[0], nk, slot, experts)
    vmem = pl.BlockSpec(memory_space=pltpu.VMEM)
    hbm = pl.BlockSpec(memory_space=pl.ANY)
    dma = pltpu.SemaphoreType.DMA
    return pl.pallas_call(
        functools.partial(kernel, cfg),
        out_shape=(
            jax.ShapeDtypeStruct((length, cols_out), BF16),
            jax.ShapeDtypeStruct((n_rows, down_cols), BF16),
        ),
        in_specs=[vmem] * 9 + [hbm] * 4,
        out_specs=(vmem, vmem),
        scratch_shapes=[
            pltpu.VMEM((ch // 128, HALO + length, 128), F32),
            pltpu.VMEM((n_tp, length, ch), BF16),
            pltpu.VMEM((length // nk, n_tp * ch), BF16),
            pltpu.VMEM((n_z, 2, n_rows, width), BF16),
            pltpu.VMEM((n_ep, extra, n_rows), BF16),
            pltpu.VMEM((2, extra, n_rows), F32),
            pltpu.VMEM((2 * slot, width), BF16),
            pltpu.VMEM((n_tp, n_z, 2 * slot, half_ff), BF16),
            pltpu.VMEM((n_z, 2 * slot, down_cols), BF16),
            pltpu.VMEM((n_ep, slot, down_cols), BF16),
            pltpu.VMEM(out_weight.shape, BF16),
            pltpu.VMEM(gate_weight.shape[1:], BF16),
            pltpu.VMEM(up_weight.shape[1:], BF16),
            pltpu.VMEM(down_weight.shape[1:], BF16),
            dma((4,)),
            dma((2,)),
            dma((3, nk)),
            dma((n_tp, nk)),
            dma((n_z, 3)),
            dma((n_z, 2)),
            dma((n_ep,)),
            dma((n_ep,)),
            dma((3, n_z, 2)),
            dma((n_tp, n_z, 2)),
            dma((n_ep,)),
            dma((n_ep,)),
        ],
        compiler_params=pltpu.CompilerParams(
            collective_id=0, has_side_effects=True, vmem_limit_bytes=62 * 1024 * 1024
        ),
    )(
        value_in,
        gate_in,
        conv_kernel,
        norm_gain.reshape(1, n_tp * ch),
        norm_shift.reshape(1, n_tp * ch),
        expert_input,
        expert_gain.reshape(1, width),
        route_ids.T,
        route_weights.T,
        out_weight,
        gate_weight,
        up_weight,
        down_weight,
    )


def solution(mesh):
    return jax.shard_map(
        body,
        mesh=mesh,
        in_specs=(
            P("ep", "tp"),
            P("ep", "tp"),
            P(None, "tp"),
            P(),
            P(),
            P(None, "tp"),
            P("ep", None),
            P(),
            P("ep", None),
            P("ep", None),
            P("ep", None, "tp"),
            P("ep", None, "tp"),
            P("ep", None, "tp"),
        ),
        out_specs=(P("ep", "tp"), P("ep", "tp")),
        check_vma=False,
    )
```
